32 devices in a mesh: kv: 16 (over z, y, x), tp: 2 (over core).
Axes of the slice: x: 2, y: 2, z: 4, core: 2. Of those that a mesh axis runs over, the one named last changes fastest.
Arguments:
- tokens: bfloat16 [256, 2048], P('kv', 'tp'), may hold values from -20 to 20
- norm_gain: float32 [2048], replicated, may hold values from 0.1 to 1.9
- w_query: bfloat16 [2048, 1024], P(None, 'tp'), may hold values from -0.125 to 0.125
- w_key: bfloat16 [2048, 1024], P(None, 'tp'), may hold values from -0.125 to 0.125
- w_value: bfloat16 [2048, 1024], P(None, 'tp'), may hold values from -0.125 to 0.125
- w_outgate: bfloat16 [2048, 1024], P(None, 'tp'), may hold values from -0.125 to 0.125
- w_input_gate: bfloat16 [2048, 8], replicated, may hold values from -0.125 to 0.125
- w_forget_gate: bfloat16 [2048, 8], replicated, may hold values from -0.125 to 0.125
- memory: float32 [256, 8, 128, 128], P('kv', 'tp'), may hold values from -6 to 6
- normalizer: float32 [256, 8, 128], P('kv', 'tp'), may hold values from -6 to 6
- memory_max: float32 [256, 8], P('kv', 'tp'), may hold values from -2 to 300
- w_output: bfloat16 [1024, 2048], P(None, 'tp'), may hold values from -0.1875 to 0.1875
- ffn_gain: float32 [2048], P('tp'), may hold values from 0.1 to 1.9
- w_gate: bfloat16 [2048, 5632], P('tp', 'kv'), may hold values from -0.125 to 0.125
- w_up: bfloat16 [2048, 5632], P('tp', 'kv'), may hold values from -0.125 to 0.125
- w_down: bfloat16 [5632, 2048], P('kv', 'tp'), may hold values from -0.078125 to 0.078125
Outputs:
- result: bfloat16 [256, 2048], P('kv', 'tp')
- new_memory: float32 [256, 8, 128, 128], P('kv', 'tp')
- new_normalizer: float32 [256, 8, 128], P('kv', 'tp')
- new_max: float32 [256, 8], P('kv', 'tp')
The draws below stay inside these ranges and needn't reach their ends.
All inputs are finite; a program needn't handle non-finite values.
Results may differ from the reference program's by a relative error of at most 0.013.
Values may be sent and summed in bfloat16 or wider, within the bound.
A program may use at most 64 MiB of HBM per device.

```python
import jax
import jax.numpy as jnp
from jax import lax

D = 2048
HEADS = 8
HEAD_DIM = 128
INNER = 1024
FF = 5632
BATCH = 256


def draw_tokens(key, part):
    key_list = jax.random.split(jax.random.fold_in(key, 11), 3)
    col_pos = jnp.arange(D, dtype=jnp.float32) / (D - 1)
    col_jitter = jnp.exp(jax.random.uniform(key_list[2], (D,), jnp.float32, jnp.log(0.7), jnp.log(1.4)))
    base_draw = jnp.clip(jax.random.normal(key_list[0], (BATCH, D), jnp.float32), -4.0, 4.0)
    rise_curve = 0.6 * jnp.exp(col_pos * jnp.log(3.0))
    row_factor = jnp.exp(jax.random.uniform(key_list[1], (BATCH,), jnp.float32, jnp.log(0.5), jnp.log(2.0)))
    full_draw = base_draw * row_factor[:, None] * (rise_curve * col_jitter)[None, :]
    return jnp.clip(full_draw, -20.0, 20.0).astype(jnp.bfloat16)


def draw_memory_max(key, part):
    key_list = jax.random.split(jax.random.fold_in(key, 23), 1)
    base_draw = jax.random.uniform(key_list[0], (BATCH, HEADS), jnp.float32, -2.0, 2.0)
    return base_draw.astype(jnp.float32)


def shard_levels(own_key, extent, cuts, low, largest):
    loudness, own = 1.0, jax.random.fold_in(own_key, 6)
    for position, blocks in cuts:
        draws = jnp.exp(jax.random.uniform(jax.random.fold_in(own, position), (blocks,), jnp.float32, low / len(cuts), largest / len(cuts)))
        loudness = loudness * jnp.repeat(draws, extent[position] // blocks).reshape([-1 if axis == position else 1 for axis in range(len(extent))])
    return loudness


def scatter_about(rng, dims, scale, reach, pieces=(), held_as=jnp.bfloat16):
    drawn = scale * jax.random.normal(rng, dims, jnp.float32)
    if pieces:
        drawn = drawn * shard_levels(rng, dims, pieces, -0.22, 0.18)
    return jnp.clip(drawn, -reach, reach).astype(held_as)


def setup_inputs(seed: int = 0) -> dict:
    seeds = jax.random.split(jax.random.key(seed), 17)
    tokens = draw_tokens(jax.random.fold_in(seeds[16], 71), 0)
    norm_gain = jnp.clip(1.0 + 0.18 * jax.random.normal(seeds[1], (D,), jnp.float32), 0.1, 1.9)
    w_query = scatter_about(seeds[2], (D, INNER), D ** -0.5, 0.125, ((1, 2),))
    w_key = scatter_about(seeds[3], (D, INNER), D ** -0.5, 0.125, ((1, 2),))
    w_value = scatter_about(seeds[4], (D, INNER), D ** -0.5, 0.125, ((1, 2),))
    w_outgate = scatter_about(seeds[5], (D, INNER), D ** -0.5, 0.125, ((1, 2),))
    w_input_gate = scatter_about(seeds[6], (D, HEADS), D ** -0.5, 0.125)
    w_forget_gate = scatter_about(seeds[7], (D, HEADS), D ** -0.5, 0.125)
    memory = scatter_about(seeds[8], (BATCH, HEADS, HEAD_DIM, HEAD_DIM), 1.0, 6.0, ((0, 16), (1, 2)), jnp.float32)
    normalizer = scatter_about(seeds[9], (BATCH, HEADS, HEAD_DIM), 1.0, 6.0, ((0, 16), (1, 2)), jnp.float32)
    memory_max = draw_memory_max(jax.random.fold_in(seeds[16], 71), 0)
    w_output = scatter_about(seeds[11], (INNER, D), INNER ** -0.5, 0.1875, ((1, 2),))
    ffn_gain = jnp.clip(1.0 + 0.18 * jax.random.normal(seeds[12], (D,), jnp.float32), 0.1, 1.9)
    w_gate = scatter_about(seeds[13], (D, FF), D ** -0.5, 0.125, ((0, 2), (1, 16)))
    w_up = scatter_about(seeds[14], (D, FF), D ** -0.5, 0.125, ((0, 2), (1, 16)))
    w_down = scatter_about(seeds[15], (FF, D), FF ** -0.5, 0.078125, ((0, 16), (1, 2)))
    return dict(tokens=tokens, norm_gain=norm_gain, w_query=w_query, w_key=w_key, w_value=w_value, w_outgate=w_outgate, w_input_gate=w_input_gate, w_forget_gate=w_forget_gate, memory=memory, normalizer=normalizer, memory_max=memory_max, w_output=w_output, ffn_gain=ffn_gain, w_gate=w_gate, w_up=w_up, w_down=w_down)


def reference(tokens, norm_gain, w_query, w_key, w_value, w_outgate, w_input_gate, w_forget_gate, memory, normalizer, memory_max, w_output, ffn_gain, w_gate, w_up, w_down):
    tokens_f = tokens.astype(jnp.float32)
    row_scale = lax.rsqrt(lax.optimization_barrier(jnp.mean(tokens_f * tokens_f, axis=-1, keepdims=True)) + 1e-06)
    normed = (tokens_f * row_scale * norm_gain).astype(jnp.bfloat16)

    def project(weight):
        return jnp.dot(normed, weight, preferred_element_type=jnp.float32).reshape(BATCH, HEADS, HEAD_DIM)
    queries = project(w_query) * HEAD_DIM ** (-0.5)
    key_vec = project(w_key)
    values = project(w_value)
    outgate = project(w_outgate)
    igate = jnp.dot(normed, w_input_gate, preferred_element_type=jnp.float32)
    lforget = jax.nn.log_sigmoid(jnp.dot(normed, w_forget_gate, preferred_element_type=jnp.float32))
    new_max = jnp.maximum(lforget + memory_max, igate)
    keep_weight = jnp.exp(lforget + memory_max - new_max)
    admit_weight = jnp.exp(igate - new_max)
    new_memory = keep_weight[..., None, None] * memory + admit_weight[..., None, None] * (key_vec[..., :, None] * values[..., None, :])
    new_normalizer = keep_weight[..., None] * normalizer + admit_weight[..., None] * key_vec
    numerator = jnp.einsum('bhd,bhdv->bhv', queries, new_memory, precision=lax.Precision.HIGHEST)
    denominator = lax.optimization_barrier(jnp.sum(queries * new_normalizer, axis=-1))
    cell_out = numerator / jnp.maximum(jnp.abs(denominator), jnp.exp(-new_max))[..., None]
    head_mean = lax.optimization_barrier(jnp.mean(cell_out, axis=-1, keepdims=True))
    centered = cell_out - head_mean
    head_var = lax.optimization_barrier(jnp.mean(centered * centered, axis=-1, keepdims=True))
    mixed = (jax.nn.sigmoid(outgate) * centered * lax.rsqrt(head_var + 1e-05)).reshape(BATCH, INNER).astype(jnp.bfloat16)
    resid = (tokens_f + jnp.dot(mixed, w_output, preferred_element_type=jnp.float32)).astype(jnp.bfloat16)
    resid_f = resid.astype(jnp.float32)
    ffn_scale = lax.rsqrt(lax.optimization_barrier(jnp.mean(resid_f * resid_f, axis=-1, keepdims=True)) + 1e-06)
    ffn_in = (resid_f * ffn_gain).astype(jnp.bfloat16)
    gate_act = ffn_scale * jnp.dot(ffn_in, w_gate, preferred_element_type=jnp.float32)
    up_act = ffn_scale * jnp.dot(ffn_in, w_up, preferred_element_type=jnp.float32)
    hidden = (jax.nn.silu(gate_act) * up_act).astype(jnp.bfloat16)
    result = (resid_f + jnp.dot(hidden, w_down, preferred_element_type=jnp.float32)).astype(jnp.bfloat16)
    return (result, new_memory, new_normalizer, new_max)
```

```python
import functools

import jax
import jax.numpy as jnp
from jax import lax
from jax.experimental import pallas as pl
from jax.experimental.pallas import tpu as pltpu
from jax.sharding import PartitionSpec as P

F32, BF16 = jnp.float32, jnp.bfloat16
MESH = pl.DeviceIdType.MESH
ANY = pl.BlockSpec(memory_space=pl.ANY)
VMEM = pl.BlockSpec(memory_space=pltpu.VMEM)
HBM = pl.BlockSpec(memory_space=pltpu.HBM)
DEPTH = 6
VMEM_BYTES = 67043328


def partner(index, bits):
    out, bit = index, 1
    while bit <= bits:
        if bits & bit:
            out = out + bit - 2 * bit * ((index // bit) % 2)
        bit *= 2
    return out


def split_groups(count):
    slow = 1
    while slow * slow < count:
        slow *= 2
    assert count % slow == 0
    return slow, count // slow


def nt_dot(a, b):
    return lax.dot_general(a, b, (((1,), (1,)), ((), ())), preferred_element_type=F32)


def step_kernel(
    nz, ny, nt, width,
    tokens_hbm, norm_gain_hbm, w_ig_hbm, w_fg_hbm, normalizer_hbm, memory_max_hbm, gain_hbm,
    w_key_hbm, w_value_hbm, w_query_hbm, w_outgate_hbm, memory_hbm, w_out_hbm, w_gate_hbm, w_up_hbm, w_down_hbm,
    out_ref, memory, new_norm, new_max_ref,
    tokens_ref, norm_gain_ref, w_ig_ref, w_fg_ref, normalizer_ref, memory_max_ref, gain_ref,
    w_key, w_value, w_query, w_outgate, w_out, w_gate, w_up, w_down,
    tok, normed, num, factors, mixed_ref, mix, rows, part, part_in, down, down_in, total, total_in, ours,
    small_sem, load_sem, tok_sem, mix_sem, zed_recv, plane_recv, gather_send,
    part_recv, part_send, down_recv, total_recv, reduce_send,
):
    k, t = lax.axis_index("kv"), lax.axis_index("tp")
    z, y = k // ny, k % ny
    n, own, cols = rows.shape
    heads, dim = memory.shape[1], memory.shape[3]
    ff = w_down.shape[0]
    pad = (part.shape[2] - 128) // 2

    def at_zed(off):
        return (partner(z, off) * ny + y, t)

    def at_plane(off):
        return (z * ny + partner(y, off), t)

    def at_tp(off):
        return (k, partner(t, off))

    smalls = [
        (tokens_hbm, tokens_ref), (norm_gain_hbm, norm_gain_ref), (w_ig_hbm, w_ig_ref), (w_fg_hbm, w_fg_ref),
        (memory_max_hbm, memory_max_ref), (normalizer_hbm, normalizer_ref), (gain_hbm, gain_ref),
    ]
    smalls = [pltpu.make_async_copy(src, dst, small_sem.at[i]) for i, (src, dst) in enumerate(smalls)]
    smalls[0].start()
    peers = [at_tp(o) for o in range(1, nt)]
    peers += [at_plane(o) for o in range(1, ny)]
    peers += [at_zed(o) for o in range(1, nz)]
    barrier = pltpu.get_barrier_semaphore()
    for peer in peers:
        pl.semaphore_signal(barrier, inc=1, device_id=peer, device_id_type=MESH)

    pairs = [(w_query_hbm, w_query), (w_key_hbm, w_key), (w_value_hbm, w_value), (w_outgate_hbm, w_outgate)]
    pairs += [(memory_hbm.at[:, h], memory.at[:, h]) for h in range(heads)]
    pairs += [(w_out_hbm, w_out), (w_gate_hbm, w_gate), (w_up_hbm, w_up), (w_down_hbm, w_down)]
    loads = [pltpu.make_async_copy(src, dst, load_sem.at[i % DEPTH]) for i, (src, dst) in enumerate(pairs)]
    for load in smalls[1:] + loads[:DEPTH]:
        load.start()

    def arrived(i):
        loads[i].wait()
        if i + DEPTH < len(loads):
            loads[i + DEPTH].start()

    def push(src, dst, send_sem, recv_sem, device):
        pltpu.make_async_remote_copy(
            src_ref=src, dst_ref=dst, send_sem=send_sem, recv_sem=recv_sem,
            device_id=device, device_id_type=MESH,
        ).start()

    def drain(ref, sem):
        pltpu.make_async_copy(ref, ref, sem).wait()

    smalls[0].wait()
    pl.semaphore_wait(barrier, len(peers))
    for o in range(1, nt):
        push(tokens_ref, tok.at[o - 1], tok_sem.at[1], tok_sem.at[0], at_tp(o))
    total_in[z] = jnp.zeros((own, cols), BF16)
    for load in smalls[1:]:
        load.wait()
    if nt > 1:
        drain(tok, tok_sem.at[0])
    blocks = [(t, tokens_ref[...].astype(F32))]
    blocks += [(partner(t, o), tok[o - 1].astype(F32)) for o in range(1, nt)]
    square = jnp.sum(blocks[0][1] * blocks[0][1], axis=-1, keepdims=True)
    for _, block in blocks[1:]:
        square = square + jnp.sum(block * block, axis=-1, keepdims=True)
    row_scale = lax.rsqrt(square / width + 1e-06)
    for owner, block in blocks:
        at = pl.ds(pl.multiple_of(owner * cols, cols), cols)
        normed[:, at] = (block * row_scale * norm_gain_ref[:, at]).astype(BF16)
    x = normed[...]
    products = []
    for i, weight in enumerate([w_query, w_key, w_value, w_outgate]):
        arrived(i)
        products.append(jnp.dot(x, weight[...], preferred_element_type=F32))
    queries, keys, values, outgates = products
    queries = queries * dim ** (-0.5)
    igates, fgates = nt_dot(w_ig_ref[...], x), nt_dot(w_fg_ref[...], x)
    diagonal = lax.broadcasted_iota(jnp.int32, (own, own), 0) == lax.broadcasted_iota(jnp.int32, (own, own), 1)

    def along(row):
        return jnp.sum(jnp.where(diagonal, row, 0.0), axis=-1, keepdims=True)

    def mine(gates):
        picked = gates[0:heads]
        for i in range(1, nt):
            picked = jnp.where(t == i, gates[i * heads : (i + 1) * heads], picked)
        return picked

    igate, forget = mine(igates), mine(fgates)
    carried = jnp.minimum(forget, 0.0) - jnp.log1p(jnp.exp(-jnp.abs(forget))) + memory_max_ref[...]
    new_max = jnp.maximum(carried, igate)
    new_max_ref[...] = new_max
    keep_row, admit_row, floor_row = jnp.exp(carried - new_max), jnp.exp(igate - new_max), jnp.exp(-new_max)
    cut = [slice(h * dim, (h + 1) * dim) for h in range(heads)]
    first = 4
    for h in range(heads):
        arrived(first + h)
    for h in range(heads):
        turned = queries[:, cut[h]].T
        for r in range(own):
            num[h, r : r + 1, :] = jnp.sum(memory[r, h] * turned[:, r : r + 1], axis=0, keepdims=True)
    for h in range(heads):
        keep = jnp.broadcast_to(along(keep_row[h : h + 1]), (own, dim))
        key, value, query = along(admit_row[h : h + 1]) * keys[:, cut[h]], values[:, cut[h]], queries[:, cut[h]]
        factors[0, h], factors[1, h], factors[2, h] = keep, key, value
        grown = keep * normalizer_ref[:, h, :] + key
        new_norm[:, h, :] = grown
        denominator = jnp.sum(query * grown, axis=-1, keepdims=True)
        match = jnp.sum(query * key, axis=-1, keepdims=True)
        numerator = keep * num[h] + match * value
        cell_out = numerator / jnp.maximum(jnp.abs(denominator), along(floor_row[h : h + 1]))
        centered = cell_out - jnp.mean(cell_out, axis=-1, keepdims=True)
        head_var = jnp.mean(centered * centered, axis=-1, keepdims=True)
        gate = 1.0 / (1.0 + jnp.exp(-outgates[:, cut[h]]))
        mixed_ref[:, cut[h]] = (gate * centered * lax.rsqrt(head_var + 1e-05)).astype(BF16)

    for o in range(1, nt):
        push(mixed_ref, mix.at[o - 1], mix_sem.at[1], mix_sem.at[0], at_tp(o))
    first += heads
    arrived(first)
    inner = mixed_ref.shape[1]

    def project(value, owner):
        return jnp.dot(value, w_out[pl.ds(pl.multiple_of(owner * inner, inner), inner), :], preferred_element_type=F32)

    acc = tokens_ref[...].astype(F32) + project(mixed_ref[...], t)
    if nt > 1:
        drain(mix, mix_sem.at[0])
    for o in range(1, nt):
        acc = acc + project(mix[o - 1], partner(t, o))
    rows[k] = acc.astype(BF16)

    def spread(source, c):
        for o in range(1, ny):
            push(rows.at[source], rows.at[source], gather_send, plane_recv.at[c], at_plane(o))

    for o in reversed(range(1, nz)):
        push(rows.at[k], rows.at[k], gather_send, zed_recv.at[z], at_zed(o))
    spread(k, z)

    def forward(c):
        @pl.when(z != c)
        def _():
            drain(rows.at[c * ny + y], zed_recv.at[c])
            spread(c * ny + y, c)

    for c in range(nz):
        forward(c)
    for h in range(heads):
        turned = factors[1, h].T
        for r in range(own):
            memory[r, h] = factors[0, h, r : r + 1] * memory[r, h] + turned[:, r : r + 1] * factors[2, h, r : r + 1]

    gates = {}
    arrived(first + 1)
    arrived(first + 2)
    arrived(first + 3)

    def stage_a(c):
        if ny > 1:
            drain(rows.at[pl.ds(0, ny - 1)], plane_recv.at[c])
        xf = rows[c * ny : (c + 1) * ny].reshape(ny * own, cols).astype(F32)
        square = jnp.sum(xf * xf, axis=-1, keepdims=True)
        h = (xf * gain_ref[...]).astype(BF16)
        gate = nt_dot(h, w_gate[...])
        up = nt_dot(h, w_up[...])
        high = square.astype(BF16).astype(F32)
        lane = lax.broadcasted_iota(jnp.int32, (ny * own, 128), 1)
        part[c, :, 0:ff] = gate.astype(BF16)
        part[c, :, pad : pad + ff] = up.astype(BF16)
        part[c, :, 2 * pad :] = jnp.where(lane < 64, high, square - high).astype(BF16)
        for o in range(1, nt):
            push(part.at[c], part_in.at[c, o - 1], part_send, part_recv.at[c], at_tp(o))
        gates[c] = (gate, up, square)

    def stage_b(c):
        gate, up, square = gates.pop(c)
        if nt > 1:
            drain(part_in.at[c], part_recv.at[c])
        for o in range(1, nt):
            gate = gate + part_in[c, o - 1, :, 0:ff].astype(F32)
            up = up + part_in[c, o - 1, :, pad : pad + ff].astype(F32)
            tail = part_in[c, o - 1, :, 2 * pad :].astype(F32)
            square = square + jnp.sum(tail, axis=-1, keepdims=True) * (1.0 / 64)
        scale = lax.rsqrt(square / width + 1e-06)
        g = scale * gate
        hidden = (g / (1.0 + jnp.exp(-g)) * (scale * up)).astype(BF16)
        out = jnp.dot(hidden, w_down[...], preferred_element_type=F32)
        down[c] = out.reshape(ny, own, cols).astype(BF16)
        for o in range(1, ny):
            push(down.at[c, partner(y, o)], down_in.at[c, o - 1], reduce_send, down_recv.at[c], at_plane(o))

    def stage_c(c):
        acc = down[c, y].astype(F32)
        if ny > 1:
            drain(rows.at[pl.ds(0, ny - 1)], down_recv.at[c])
        for o in range(1, ny):
            acc = acc + down_in[c, o - 1].astype(F32)

        @pl.when(z == c)
        def _():
            ours[...] = acc

        @pl.when(z != c)
        def _():
            total[c] = acc.astype(BF16)
            push(total.at[c], total_in.at[z], reduce_send, total_recv, (c * ny + y, t))

    stage_a(0)
    for c in range(1, nz + 1):
        if c < nz:
            stage_a(c)
        stage_b(c - 1)
    for c in range(nz):
        stage_c(c)
    acc = rows[k].astype(F32) + ours[...]
    if nz > 1:
        drain(rows.at[pl.ds(0, nz - 1)], total_recv)
    for c in range(nz):
        acc = acc + total_in[c].astype(F32)
    out_ref[...] = acc.astype(BF16)
    if n > 1:
        drain(rows.at[pl.ds(0, n - 1)], gather_send)
        drain(rows.at[pl.ds(0, n - 1)], reduce_send)
    if nt > 1:
        drain(tok, tok_sem.at[1])
        drain(mix, mix_sem.at[1])
        drain(part_in, part_send)


def store_kernel(result, memory, normalizer, new_max, result_hbm, memory_hbm, normalizer_hbm, new_max_hbm, sem):
    pairs = [(memory, memory_hbm), (normalizer, normalizer_hbm), (new_max, new_max_hbm), (result, result_hbm)]
    copies = [pltpu.make_async_copy(src, dst, sem.at[i]) for i, (src, dst) in enumerate(pairs)]
    for copy in copies:
        copy.start()
    for copy in copies:
        copy.wait()


def per_device(
    mesh, tokens, norm_gain, w_query, w_key, w_value, w_outgate, w_input_gate, w_forget_gate,
    memory, normalizer, memory_max, w_output, ffn_gain, w_gate, w_up, w_down,
):
    n, nt = mesh.shape["kv"], mesh.shape["tp"]
    nz, ny = split_groups(n)
    own, cols = tokens.shape
    heads, dim = memory.shape[1], memory.shape[2]
    inner = heads * dim
    ff = w_down.shape[0]
    pad = -(-ff // 128) * 128
    dma = pltpu.SemaphoreType.DMA
    peers = max(nt - 1, 1)
    w_gate, w_up = w_gate.T, w_up.T
    vm = lambda like: pltpu.VMEM(like.shape, like.dtype)
    kept = 4 * (memory.size + 2 * normalizer.size) + 2 * tokens.size
    result, new_memory, new_normalizer, new_max = pl.pallas_call(
        functools.partial(step_kernel, nz, ny, nt, cols * nt),
        out_shape=(
            pltpu.VMEM((own, cols), BF16),
            pltpu.VMEM(memory.shape, F32),
            pltpu.VMEM(normalizer.shape, F32),
            pltpu.VMEM((heads, own), F32),
        ),
        in_specs=[HBM] * 16,
        out_specs=(VMEM,) * 4,
        scratch_shapes=[
            vm(tokens), pltpu.VMEM((1, cols * nt), F32), pltpu.VMEM(w_input_gate.shape[::-1], BF16),
            pltpu.VMEM(w_forget_gate.shape[::-1], BF16), vm(normalizer), pltpu.VMEM((heads, own), F32),
            pltpu.VMEM((1, cols), F32),
            vm(w_key), vm(w_value), vm(w_query), vm(w_outgate),
            vm(w_output), vm(w_gate), vm(w_up), vm(w_down),
            pltpu.VMEM((peers, own, cols), BF16),
            pltpu.VMEM((own, cols * nt), BF16),
            pltpu.VMEM((heads, own, dim), F32),
            pltpu.VMEM((3, heads, own, dim), F32),
            pltpu.VMEM((own, inner), BF16),
            pltpu.VMEM((peers, own, inner), BF16),
            pltpu.VMEM((n, own, cols), BF16),
            pltpu.VMEM((nz, ny * own, 2 * pad + 128), BF16),
            pltpu.VMEM((nz, peers, ny * own, 2 * pad + 128), BF16),
            pltpu.VMEM((nz, ny, own, cols), BF16),
            pltpu.VMEM((nz, max(ny - 1, 1), own, cols), BF16),
            pltpu.VMEM((nz, own, cols), BF16),
            pltpu.VMEM((nz, own, cols), BF16),
            pltpu.VMEM((own, cols), F32),
            dma((7,)),
            dma((DEPTH,)),
            dma((2,)),
            dma((2,)),
            dma((nz,)),
            dma((nz,)),
            dma,
            dma((nz,)),
            dma,
            dma((nz,)),
            dma,
            dma,
        ],
        compiler_params=pltpu.CompilerParams(collective_id=0, has_side_effects=True, vmem_limit_bytes=VMEM_BYTES - kept),
        name="decode_step",
    )(
        tokens, norm_gain.reshape(1, -1), w_input_gate.T, w_forget_gate.T, normalizer, memory_max.T,
        ffn_gain.reshape(1, cols), w_key, w_value, w_query, w_outgate, memory, w_output, w_gate, w_up, w_down,
    )
    result, new_memory, new_normalizer, new_max = pl.pallas_call(
        store_kernel,
        out_shape=(
            jax.ShapeDtypeStruct(tokens.shape, BF16),
            jax.ShapeDtypeStruct(memory.shape, F32),
            jax.ShapeDtypeStruct(normalizer.shape, F32),
            jax.ShapeDtypeStruct((heads, own), F32),
        ),
        in_specs=[VMEM] * 4,
        out_specs=(HBM,) * 4,
        scratch_shapes=[dma((4,))],
        compiler_params=pltpu.CompilerParams(vmem_limit_bytes=2**20),
        name="store",
    )(result, new_memory, new_normalizer, new_max)
    return (result, new_memory, new_normalizer, new_max.T)


def solution(mesh):
    placed = (
        P("kv", "tp"),
        P(),
        P(None, "tp"),
        P(None, "tp"),
        P(None, "tp"),
        P(None, "tp"),
        P(),
        P(),
        P("kv", "tp", None, None),
        P("kv", "tp", None),
        P("kv", "tp"),
        P(None, "tp"),
        P("tp"),
        P("tp", "kv"),
        P("tp", "kv"),
        P("kv", "tp"),
    )
    return jax.shard_map(
        functools.partial(per_device, mesh),
        mesh=mesh,
        in_specs=placed,
        out_specs=(P("kv", "tp"), P("kv", "tp", None, None), P("kv", "tp", None), P("kv", "tp")),
        check_vma=False,
    )
```

```python
import functools

import jax
import jax.numpy as jnp
from jax import lax
from jax.experimental import pallas as pl
from jax.experimental.pallas import tpu as pltpu
from jax.sharding import PartitionSpec as P

F32, BF16 = jnp.float32, jnp.bfloat16
MESH = pl.DeviceIdType.MESH
ANY = pl.BlockSpec(memory_space=pl.ANY)
VMEM = pl.BlockSpec(memory_space=pltpu.VMEM)
HBM = pl.BlockSpec(memory_space=pltpu.HBM)
DEPTH = 8
VMEM_BYTES = 67043328


def partner(index, bits):
    out, bit = index, 1
    while bit <= bits:
        if bits & bit:
            out = out + bit - 2 * bit * ((index // bit) % 2)
        bit *= 2
    return out


def split_groups(count):
    slow = 1
    while slow * slow < count:
        slow *= 2
    assert count % slow == 0
    return slow, count // slow


def nt_dot(a, b):
    return lax.dot_general(a, b, (((1,), (1,)), ((), ())), preferred_element_type=F32)


def step_kernel(
    nz, ny, nt, width,
    tokens_hbm, norm_gain_hbm, w_ig_hbm, w_fg_hbm, normalizer_hbm, memory_max_hbm, gain_hbm,
    w_key_hbm, w_value_hbm, w_query_hbm, w_outgate_hbm, memory_hbm, w_out_hbm, w_gate_hbm, w_up_hbm, w_down_hbm,
    out_ref, memory, new_norm, new_max_ref,
    tokens_ref, norm_gain_ref, w_ig_ref, w_fg_ref, normalizer_ref, memory_max_ref, gain_ref,
    w_key, w_value, w_query, w_outgate, w_out, w_gate, w_up, w_down,
    tok, normed, num, factors, mixed_ref, mix, rows, part, part_in, down, down_in, total, total_in, ours,
    small_sem, load_sem, tok_sem, mix_sem, zed_recv, plane_recv, gather_send,
    part_recv, part_send, down_recv, total_recv, reduce_send, ahead_sem, behind_sem,
):
    k, t = lax.axis_index("kv"), lax.axis_index("tp")
    z, y = k // ny, k % ny
    n, own, cols = rows.shape
    heads, dim = memory.shape[1], memory.shape[3]
    ff = w_down.shape[0]
    pad = (part.shape[2] - 128) // 2
    plane_order = sorted(range(1, ny), key=lambda o: -bin(o).count("1"))

    def at_plane(off):
        return (z * ny + partner(y, off), t)

    def at_tp(off):
        return (k, partner(t, off))

    smalls = [
        (tokens_hbm, tokens_ref), (norm_gain_hbm, norm_gain_ref), (w_ig_hbm, w_ig_ref), (w_fg_hbm, w_fg_ref),
        (memory_max_hbm, memory_max_ref), (normalizer_hbm, normalizer_ref), (gain_hbm, gain_ref),
    ]
    smalls = [pltpu.make_async_copy(src, dst, small_sem.at[i]) for i, (src, dst) in enumerate(smalls)]
    smalls[0].start()
    smalls[1].start()
    peers = [at_tp(o) for o in range(1, nt)]
    peers += [at_plane(o) for o in range(1, ny)]
    barrier = pltpu.get_barrier_semaphore()

    def at_step(d):
        return ((z + d) * ny + y, t)

    def greet(sem, device):
        pl.semaphore_signal(sem, inc=1, device_id=device, device_id_type=MESH)

    for peer in peers:
        greet(barrier, peer)
    if nz > 1:
        pl.when(z + 1 < nz)(lambda: greet(barrier, at_step(1)))
        pl.when(z >= 1)(lambda: greet(barrier, at_step(-1)))

    def tell(d):
        pl.when((z >= 1) & (z + d < nz))(lambda: greet(ahead_sem.at[d + 1], at_step(-1)))
        pl.when((z + 1 < nz) & (z >= d))(lambda: greet(behind_sem.at[d + 1], at_step(1)))

    def hear(d):
        pl.when(z + d < nz)(lambda: pl.semaphore_wait(ahead_sem.at[d], 1))
        pl.when(z >= d)(lambda: pl.semaphore_wait(behind_sem.at[d], 1))
        if d + 1 < nz:
            tell(d)

    pairs = [(w_query_hbm, w_query)]
    pairs += [(memory_hbm.at[:, h], memory.at[:, h]) for h in range(heads)]
    pairs += [(w_key_hbm, w_key), (w_value_hbm, w_value), (w_outgate_hbm, w_outgate)]
    pairs += [(w_out_hbm, w_out), (w_gate_hbm, w_gate), (w_up_hbm, w_up), (w_down_hbm, w_down)]
    loads = [pltpu.make_async_copy(src, dst, load_sem.at[i % DEPTH]) for i, (src, dst) in enumerate(pairs)]
    for load in loads[:1] + smalls[2:] + loads[1:DEPTH]:
        load.start()

    def arrived(i):
        loads[i].wait()
        if i + DEPTH < len(loads):
            loads[i + DEPTH].start()

    def push(src, dst, send_sem, recv_sem, device):
        pltpu.make_async_remote_copy(
            src_ref=src, dst_ref=dst, send_sem=send_sem, recv_sem=recv_sem,
            device_id=device, device_id_type=MESH,
        ).start()

    def drain(ref, sem):
        pltpu.make_async_copy(ref, ref, sem).wait()

    smalls[0].wait()
    pl.semaphore_wait(barrier, len(peers) + (2 * nz - 2 - z) // nz + (z + nz - 1) // nz)
    for o in range(1, nt):
        push(tokens_ref, tok.at[o - 1], tok_sem.at[1], tok_sem.at[0], at_tp(o))
    if nz > 2:
        tell(1)
    total_in[z] = jnp.zeros((own, cols), BF16)
    smalls[1].wait()
    if nt > 1:
        drain(tok, tok_sem.at[0])
    blocks = [(t, tokens_ref[...].astype(F32))]
    blocks += [(partner(t, o), tok[o - 1].astype(F32)) for o in range(1, nt)]
    square = jnp.sum(blocks[0][1] * blocks[0][1], axis=-1, keepdims=True)
    for _, block in blocks[1:]:
        square = square + jnp.sum(block * block, axis=-1, keepdims=True)
    row_scale = lax.rsqrt(square / width + 1e-06)
    for owner, block in blocks:
        at = pl.ds(pl.multiple_of(owner * cols, cols), cols)
        normed[:, at] = (block * row_scale * norm_gain_ref[:, at]).astype(BF16)
    x = normed[...]
    cut = [slice(h * dim, (h + 1) * dim) for h in range(heads)]

    def projected(i, weight):
        arrived(i)
        return jnp.dot(x, weight[...], preferred_element_type=F32)

    def recall(some):
        for h in some:
            turned = queries[:, cut[h]].T
            for r in range(own):
                num[h, r : r + 1, :] = jnp.sum(memory[r, h] * turned[:, r : r + 1], axis=0, keepdims=True)

    queries = projected(0, w_query) * dim ** (-0.5)
    for h in range(heads):
        arrived(1 + h)
    first = 1 + heads
    third = -(-heads // 3)
    keys = projected(first, w_key)
    recall(range(heads)[:third])
    values = projected(first + 1, w_value)
    recall(range(heads)[third : heads - heads // 3])
    if nz > 2:
        hear(2)
    for load in smalls[2:]:
        load.wait()
    outgates = projected(first + 2, w_outgate)
    recall(range(heads)[heads - heads // 3 :])
    igates, fgates = nt_dot(w_ig_ref[...], x), nt_dot(w_fg_ref[...], x)
    diagonal = lax.broadcasted_iota(jnp.int32, (own, own), 0) == lax.broadcasted_iota(jnp.int32, (own, own), 1)

    def along(row):
        return jnp.sum(jnp.where(diagonal, row, 0.0), axis=-1, keepdims=True)

    def mine(gates):
        picked = gates[0:heads]
        for i in range(1, nt):
            picked = jnp.where(t == i, gates[i * heads : (i + 1) * heads], picked)
        return picked

    igate, forget = mine(igates), mine(fgates)
    carried = jnp.minimum(forget, 0.0) - jnp.log1p(jnp.exp(-jnp.abs(forget))) + memory_max_ref[...]
    new_max = jnp.maximum(carried, igate)
    new_max_ref[...] = new_max
    keep_row, admit_row, floor_row = jnp.exp(carried - new_max), jnp.exp(igate - new_max), jnp.exp(-new_max)
    for h in range(heads):
        keep = jnp.broadcast_to(along(keep_row[h : h + 1]), (own, dim))
        key, value, query = along(admit_row[h : h + 1]) * keys[:, cut[h]], values[:, cut[h]], queries[:, cut[h]]
        factors[0, h], factors[1, h], factors[2, h] = keep, key, value
        grown = keep * normalizer_ref[:, h, :] + key
        new_norm[:, h, :] = grown
        denominator = jnp.sum(query * grown, axis=-1, keepdims=True)
        match = jnp.sum(query * key, axis=-1, keepdims=True)
        numerator = keep * num[h] + match * value
        cell_out = numerator / jnp.maximum(jnp.abs(denominator), along(floor_row[h : h + 1]))
        centered = cell_out - jnp.mean(cell_out, axis=-1, keepdims=True)
        head_var = jnp.mean(centered * centered, axis=-1, keepdims=True)
        gate = 1.0 / (1.0 + jnp.exp(-outgates[:, cut[h]]))
        mixed_ref[:, cut[h]] = (gate * centered * lax.rsqrt(head_var + 1e-05)).astype(BF16)

    for o in range(1, nt):
        push(mixed_ref, mix.at[o - 1], mix_sem.at[1], mix_sem.at[0], at_tp(o))
    first += 3
    arrived(first)
    inner = mixed_ref.shape[1]

    def project(value, owner):
        return jnp.dot(value, w_out[pl.ds(pl.multiple_of(owner * inner, inner), inner), :], preferred_element_type=F32)

    acc = tokens_ref[...].astype(F32) + project(mixed_ref[...], t)
    if nt > 1:
        drain(mix, mix_sem.at[0])
    for o in range(1, nt):
        acc = acc + project(mix[o - 1], partner(t, o))
    rows[k] = acc.astype(BF16)

    def spread(source, c):
        for o in plane_order:
            push(rows.at[source], rows.at[source], gather_send, plane_recv.at[c], at_plane(o))

    for d in range(3, nz):
        hear(d)

    def offer(c):
        push(rows.at[k], rows.at[k], gather_send, zed_recv.at[z], (c * ny + y, t))

    for d in reversed(range(1, nz)):
        pl.when(z + d < nz)(functools.partial(offer, z + d))
        pl.when(z >= d)(functools.partial(offer, z - d))
    spread(k, z)
    for h in range(heads):
        turned = factors[1, h].T
        for r in range(own):
            memory[r, h] = factors[0, h, r : r + 1] * memory[r, h] + turned[:, r : r + 1] * factors[2, h, r : r + 1]

    def chunk(j):
        return j - 1 + (nz + j - 1 - z) // nz if j else z

    def forward(j):
        c = chunk(j)
        drain(rows.at[c * ny + y], zed_recv.at[c])
        spread(c * ny + y, c)

    gates = {}
    arrived(first + 1)
    arrived(first + 2)
    arrived(first + 3)

    def stage_a(c):
        if ny > 1:
            drain(rows.at[pl.ds(0, ny - 1)], plane_recv.at[chunk(c)])
        xf = rows[pl.ds(chunk(c) * ny, ny)].reshape(ny * own, cols).astype(F32)
        square = jnp.sum(xf * xf, axis=-1, keepdims=True)
        h = (xf * gain_ref[...]).astype(BF16)
        gate = nt_dot(h, w_gate[...])
        up = nt_dot(h, w_up[...])
        high = square.astype(BF16).astype(F32)
        lane = lax.broadcasted_iota(jnp.int32, (ny * own, 128), 1)
        part[c, :, 0:ff] = gate.astype(BF16)
        part[c, :, pad : pad + ff] = up.astype(BF16)
        part[c, :, 2 * pad :] = jnp.where(lane < 64, high, square - high).astype(BF16)
        for o in range(1, nt):
            push(part.at[c], part_in.at[c, o - 1], part_send, part_recv.at[c], at_tp(o))
        gates[c] = (gate, up, square)

    def stage_b(c):
        gate, up, square = gates.pop(c)
        if nt > 1:
            drain(part_in.at[c], part_recv.at[c])
        for o in range(1, nt):
            gate = gate + part_in[c, o - 1, :, 0:ff].astype(F32)
            up = up + part_in[c, o - 1, :, pad : pad + ff].astype(F32)
            tail = part_in[c, o - 1, :, 2 * pad :].astype(F32)
            square = square + jnp.sum(tail, axis=-1, keepdims=True) * (1.0 / 64)
        scale = lax.rsqrt(square / width + 1e-06)
        g = scale * gate
        hidden = (g / (1.0 + jnp.exp(-g)) * (scale * up)).astype(BF16)
        out = jnp.dot(hidden, w_down[...], preferred_element_type=F32)
        down[c] = out.reshape(ny, own, cols).astype(BF16)
        for o in plane_order:
            push(down.at[c, partner(y, o)], down_in.at[c, o - 1], reduce_send, down_recv.at[c], at_plane(o))

    def stage_c(c):
        acc = down[c, y].astype(F32)
        if ny > 1:
            drain(rows.at[pl.ds(0, ny - 1)], down_recv.at[c])
        for o in range(1, ny):
            acc = acc + down_in[c, o - 1].astype(F32)

        if c == 0:
            ours[...] = acc
        else:
            total[c] = acc.astype(BF16)
            push(total.at[c], total_in.at[z], reduce_send, total_recv, (chunk(c) * ny + y, t))

    if nz > 1:
        forward(1)
    stage_a(0)
    for j in range(2, nz):
        forward(j)
    stage_b(0)
    for j in range(1, nz + 1):
        if j < nz:
            stage_a(j)
        if j > 1:
            stage_b(j - 1)
    for j in range(1, nz):
        stage_c(j)
    stage_c(0)
    acc = rows[k].astype(F32) + ours[...]
    if nz > 1:
        drain(rows.at[pl.ds(0, nz - 1)], total_recv)
    for c in range(nz):
        acc = acc + total_in[c].astype(F32)
    out_ref[...] = acc.astype(BF16)
    if n > 1:
        drain(rows.at[pl.ds(0, n - 1)], gather_send)
        drain(rows.at[pl.ds(0, n - 1)], reduce_send)
    if nt > 1:
        drain(tok, tok_sem.at[1])
        drain(mix, mix_sem.at[1])
        drain(part_in, part_send)


def store_kernel(result, memory, normalizer, new_max, result_hbm, memory_hbm, normalizer_hbm, new_max_hbm, sem):
    pairs = [(memory, memory_hbm), (normalizer, normalizer_hbm), (new_max, new_max_hbm), (result, result_hbm)]
    copies = [pltpu.make_async_copy(src, dst, sem.at[i]) for i, (src, dst) in enumerate(pairs)]
    for copy in copies:
        copy.start()
    for copy in copies:
        copy.wait()


def per_device(
    mesh, tokens, norm_gain, w_query, w_key, w_value, w_outgate, w_input_gate, w_forget_gate,
    memory, normalizer, memory_max, w_output, ffn_gain, w_gate, w_up, w_down,
):
    n, nt = mesh.shape["kv"], mesh.shape["tp"]
    nz, ny = split_groups(n)
    own, cols = tokens.shape
    heads, dim = memory.shape[1], memory.shape[2]
    inner = heads * dim
    ff = w_down.shape[0]
    pad = -(-ff // 128) * 128
    dma = pltpu.SemaphoreType.DMA
    peers = max(nt - 1, 1)
    w_gate, w_up = w_gate.T, w_up.T
    vm = lambda like: pltpu.VMEM(like.shape, like.dtype)
    kept = 4 * (memory.size + 2 * normalizer.size) + 2 * tokens.size
    result, new_memory, new_normalizer, new_max = pl.pallas_call(
        functools.partial(step_kernel, nz, ny, nt, cols * nt),
        out_shape=(
            pltpu.VMEM((own, cols), BF16),
            pltpu.VMEM(memory.shape, F32),
            pltpu.VMEM(normalizer.shape, F32),
            pltpu.VMEM((heads, own), F32),
        ),
        in_specs=[HBM] * 16,
        out_specs=(VMEM,) * 4,
        scratch_shapes=[
            vm(tokens), pltpu.VMEM((1, cols * nt), F32), pltpu.VMEM(w_input_gate.shape[::-1], BF16),
            pltpu.VMEM(w_forget_gate.shape[::-1], BF16), vm(normalizer), pltpu.VMEM((heads, own), F32),
            pltpu.VMEM((1, cols), F32),
            vm(w_key), vm(w_value), vm(w_query), vm(w_outgate),
            vm(w_output), vm(w_gate), vm(w_up), vm(w_down),
            pltpu.VMEM((peers, own, cols), BF16),
            pltpu.VMEM((own, cols * nt), BF16),
            pltpu.VMEM((heads, own, dim), F32),
            pltpu.VMEM((3, heads, own, dim), F32),
            pltpu.VMEM((own, inner), BF16),
            pltpu.VMEM((peers, own, inner), BF16),
            pltpu.VMEM((n, own, cols), BF16),
            pltpu.VMEM((nz, ny * own, 2 * pad + 128), BF16),
            pltpu.VMEM((nz, peers, ny * own, 2 * pad + 128), BF16),
            pltpu.VMEM((nz, ny, own, cols), BF16),
            pltpu.VMEM((nz, max(ny - 1, 1), own, cols), BF16),
            pltpu.VMEM((nz, own, cols), BF16),
            pltpu.VMEM((nz, own, cols), BF16),
            pltpu.VMEM((own, cols), F32),
            dma((7,)),
            dma((DEPTH,)),
            dma((2,)),
            dma((2,)),
            dma((nz,)),
            dma((nz,)),
            dma,
            dma((nz,)),
            dma,
            dma((nz,)),
            dma,
            dma,
            pltpu.SemaphoreType.REGULAR((nz,)),
            pltpu.SemaphoreType.REGULAR((nz,)),
        ],
        compiler_params=pltpu.CompilerParams(collective_id=0, has_side_effects=True, vmem_limit_bytes=VMEM_BYTES - kept),
        name="decode_step",
    )(
        tokens, norm_gain.reshape(1, -1), w_input_gate.T, w_forget_gate.T, normalizer, memory_max.T,
        ffn_gain.reshape(1, cols), w_key, w_value, w_query, w_outgate, memory, w_output, w_gate, w_up, w_down,
    )
    result, new_memory, new_normalizer, new_max = pl.pallas_call(
        store_kernel,
        out_shape=(
            jax.ShapeDtypeStruct(tokens.shape, BF16),
            jax.ShapeDtypeStruct(memory.shape, F32),
            jax.ShapeDtypeStruct(normalizer.shape, F32),
            jax.ShapeDtypeStruct((heads, own), F32),
        ),
        in_specs=[VMEM] * 4,
        out_specs=(HBM,) * 4,
        scratch_shapes=[dma((4,))],
        compiler_params=pltpu.CompilerParams(vmem_limit_bytes=2**20),
        name="store",
    )(result, new_memory, new_normalizer, new_max)
    return (result, new_memory, new_normalizer, new_max.T)


def solution(mesh):
    placed = (
        P("kv", "tp"),
        P(),
        P(None, "tp"),
        P(None, "tp"),
        P(None, "tp"),
        P(None, "tp"),
        P(),
        P(),
        P("kv", "tp", None, None),
        P("kv", "tp", None),
        P("kv", "tp"),
        P(None, "tp"),
        P("tp"),
        P("tp", "kv"),
        P("tp", "kv"),
        P("kv", "tp"),
    )
    return jax.shard_map(
        functools.partial(per_device, mesh),
        mesh=mesh,
        in_specs=placed,
        out_specs=(P("kv", "tp"), P("kv", "tp", None, None), P("kv", "tp", None), P("kv", "tp")),
        check_vma=False,
    )
```

```python
import functools

import jax
import jax.numpy as jnp
from jax import lax
from jax.experimental import pallas as pl
from jax.experimental.pallas import tpu as pltpu
from jax.sharding import PartitionSpec as P

F32, BF16 = jnp.float32, jnp.bfloat16
MESH = pl.DeviceIdType.MESH
ANY = pl.BlockSpec(memory_space=pl.ANY)
VMEM = pl.BlockSpec(memory_space=pltpu.VMEM)
HBM = pl.BlockSpec(memory_space=pltpu.HBM)
DEPTH = 8
VMEM_BYTES = 67043328


def partner(index, bits):
    out, bit = index, 1
    while bit <= bits:
        if bits & bit:
            out = out + bit - 2 * bit * ((index // bit) % 2)
        bit *= 2
    return out


def split_groups(count):
    slow = 1
    while slow * slow < count:
        slow *= 2
    assert count % slow == 0
    return slow, count // slow


def parts_of(width, count):
    count = max(1, min(count, width // 128))
    step = width // count
    return [slice(i * step, (i + 1) * step) for i in range(count)]


def nt_dot(a, b):
    return lax.dot_general(a, b, (((1,), (1,)), ((), ())), preferred_element_type=F32)


def step_kernel(
    nz, ny, nt, width,
    tokens_hbm, norm_gain_hbm, w_ig_hbm, w_fg_hbm, normalizer_hbm, memory_max_hbm, gain_hbm,
    w_key_hbm, w_value_hbm, w_query_hbm, w_outgate_hbm, memory_hbm, w_out_hbm, w_gate_hbm, w_up_hbm, w_down_hbm,
    out_ref, memory, new_norm, new_max_ref,
    tokens_ref, norm_gain_ref, w_ig_ref, w_fg_ref, normalizer_ref, memory_max_ref, gain_ref,
    w_key, w_value, w_query, w_outgate, w_out, w_gate, w_up, w_down,
    tok, normed, num, factors, mixed_ref, mix, rows, part, part_in, down, down_in, total, total_in, ours,
    small_sem, load_sem, tok_sem, mix_sem, zed_recv, plane_recv, gather_send,
    part_recv, part_send, down_recv, total_recv, reduce_send, ahead_sem, behind_sem,
):
    k, t = lax.axis_index("kv"), lax.axis_index("tp")
    z, y = k // ny, k % ny
    n, own, cols = rows.shape
    heads, dim = memory.shape[1], memory.shape[3]
    ff = w_down.shape[0]
    pad = (part.shape[2] - 128) // 2
    gather_parts, reduce_parts = parts_of(cols, 2), parts_of(cols, 2)
    plane_order = sorted(range(1, ny), key=lambda o: -bin(o).count("1"))

    def at_plane(off):
        return (z * ny + partner(y, off), t)

    def at_tp(off):
        return (k, partner(t, off))

    smalls = [
        (tokens_hbm, tokens_ref), (norm_gain_hbm, norm_gain_ref), (w_ig_hbm, w_ig_ref), (w_fg_hbm, w_fg_ref),
        (memory_max_hbm, memory_max_ref), (normalizer_hbm, normalizer_ref), (gain_hbm, gain_ref),
    ]
    smalls = [pltpu.make_async_copy(src, dst, small_sem.at[i]) for i, (src, dst) in enumerate(smalls)]
    smalls[0].start()
    smalls[1].start()
    peers = [at_tp(o) for o in range(1, nt)]
    peers += [at_plane(o) for o in range(1, ny)]
    barrier = pltpu.get_barrier_semaphore()

    def at_step(d):
        return ((z + d) * ny + y, t)

    def greet(sem, device):
        pl.semaphore_signal(sem, inc=1, device_id=device, device_id_type=MESH)

    for peer in peers:
        greet(barrier, peer)
    if nz > 1:
        pl.when(z + 1 < nz)(lambda: greet(barrier, at_step(1)))
        pl.when(z >= 1)(lambda: greet(barrier, at_step(-1)))

    def tell(d):
        pl.when((z >= 1) & (z + d < nz))(lambda: greet(ahead_sem.at[d + 1], at_step(-1)))
        pl.when((z + 1 < nz) & (z >= d))(lambda: greet(behind_sem.at[d + 1], at_step(1)))

    def hear(d):
        pl.when(z + d < nz)(lambda: pl.semaphore_wait(ahead_sem.at[d], 1))
        pl.when(z >= d)(lambda: pl.semaphore_wait(behind_sem.at[d], 1))
        if d + 1 < nz:
            tell(d)

    pairs = [(w_query_hbm, w_query)]
    pairs += [(memory_hbm.at[:, h], memory.at[:, h]) for h in range(heads)]
    pairs += [(w_key_hbm, w_key), (w_value_hbm, w_value), (w_outgate_hbm, w_outgate)]
    pairs += [(w_out_hbm, w_out), (w_gate_hbm, w_gate), (w_up_hbm, w_up), (w_down_hbm, w_down)]
    loads = [pltpu.make_async_copy(src, dst, load_sem.at[i % DEPTH]) for i, (src, dst) in enumerate(pairs)]
    for load in loads[:1] + smalls[2:] + loads[1:DEPTH]:
        load.start()

    def arrived(i):
        loads[i].wait()
        if i + DEPTH < len(loads):
            loads[i + DEPTH].start()

    def push(src, dst, send_sem, recv_sem, device):
        pltpu.make_async_remote_copy(
            src_ref=src, dst_ref=dst, send_sem=send_sem, recv_sem=recv_sem,
            device_id=device, device_id_type=MESH,
        ).start()

    def drain(ref, sem):
        pltpu.make_async_copy(ref, ref, sem).wait()

    smalls[0].wait()
    pl.semaphore_wait(barrier, len(peers) + (2 * nz - 2 - z) // nz + (z + nz - 1) // nz)
    for o in range(1, nt):
        push(tokens_ref, tok.at[o - 1], tok_sem.at[1], tok_sem.at[0], at_tp(o))
    if nz > 2:
        tell(1)
    total_in[z] = jnp.zeros((own, cols), BF16)
    smalls[1].wait()
    if nt > 1:
        drain(tok, tok_sem.at[0])
    blocks = [(t, tokens_ref[...].astype(F32))]
    blocks += [(partner(t, o), tok[o - 1].astype(F32)) for o in range(1, nt)]
    square = jnp.sum(blocks[0][1] * blocks[0][1], axis=-1, keepdims=True)
    for _, block in blocks[1:]:
        square = square + jnp.sum(block * block, axis=-1, keepdims=True)
    row_scale = lax.rsqrt(square / width + 1e-06)
    for owner, block in blocks:
        at = pl.ds(pl.multiple_of(owner * cols, cols), cols)
        normed[:, at] = (block * row_scale * norm_gain_ref[:, at]).astype(BF16)
    x = normed[...]
    cut = [slice(h * dim, (h + 1) * dim) for h in range(heads)]

    def projected(i, weight):
        arrived(i)
        return jnp.dot(x, weight[...], preferred_element_type=F32)

    def recall(some):
        for h in some:
            turned = queries[:, cut[h]].T
            for r in range(own):
                num[h, r : r + 1, :] = jnp.sum(memory[r, h] * turned[:, r : r + 1], axis=0, keepdims=True)

    queries = projected(0, w_query) * dim ** (-0.5)
    for h in range(heads):
        arrived(1 + h)
    first = 1 + heads
    third = -(-heads // 3)
    keys = projected(first, w_key)
    recall(range(heads)[:third])
    values = projected(first + 1, w_value)
    recall(range(heads)[third : heads - heads // 3])
    if nz > 2:
        hear(2)
    for load in smalls[2:]:
        load.wait()
    outgates = projected(first + 2, w_outgate)
    recall(range(heads)[heads - heads // 3 :])
    igates, fgates = nt_dot(w_ig_ref[...], x), nt_dot(w_fg_ref[...], x)
    diagonal = lax.broadcasted_iota(jnp.int32, (own, own), 0) == lax.broadcasted_iota(jnp.int32, (own, own), 1)

    def along(row):
        return jnp.sum(jnp.where(diagonal, row, 0.0), axis=-1, keepdims=True)

    def mine(gates):
        picked = gates[0:heads]
        for i in range(1, nt):
            picked = jnp.where(t == i, gates[i * heads : (i + 1) * heads], picked)
        return picked

    igate, forget = mine(igates), mine(fgates)
    carried = jnp.minimum(forget, 0.0) - jnp.log1p(jnp.exp(-jnp.abs(forget))) + memory_max_ref[...]
    new_max = jnp.maximum(carried, igate)
    new_max_ref[...] = new_max
    keep_row, admit_row, floor_row = jnp.exp(carried - new_max), jnp.exp(igate - new_max), jnp.exp(-new_max)
    for h in range(heads):
        keep = jnp.broadcast_to(along(keep_row[h : h + 1]), (own, dim))
        key, value, query = along(admit_row[h : h + 1]) * keys[:, cut[h]], values[:, cut[h]], queries[:, cut[h]]
        factors[0, h], factors[1, h], factors[2, h] = keep, key, value
        grown = keep * normalizer_ref[:, h, :] + key
        new_norm[:, h, :] = grown
        denominator = jnp.sum(query * grown, axis=-1, keepdims=True)
        match = jnp.sum(query * key, axis=-1, keepdims=True)
        numerator = keep * num[h] + match * value
        cell_out = numerator / jnp.maximum(jnp.abs(denominator), along(floor_row[h : h + 1]))
        centered = cell_out - jnp.mean(cell_out, axis=-1, keepdims=True)
        head_var = jnp.mean(centered * centered, axis=-1, keepdims=True)
        gate = 1.0 / (1.0 + jnp.exp(-outgates[:, cut[h]]))
        mixed_ref[:, cut[h]] = (gate * centered * lax.rsqrt(head_var + 1e-05)).astype(BF16)

    for o in range(1, nt):
        push(mixed_ref, mix.at[o - 1], mix_sem.at[1], mix_sem.at[0], at_tp(o))
    first += 3
    arrived(first)
    inner = mixed_ref.shape[1]

    def project(value, owner):
        return jnp.dot(value, w_out[pl.ds(pl.multiple_of(owner * inner, inner), inner), :], preferred_element_type=F32)

    acc = tokens_ref[...].astype(F32) + project(mixed_ref[...], t)
    if nt > 1:
        drain(mix, mix_sem.at[0])
    for o in range(1, nt):
        acc = acc + project(mix[o - 1], partner(t, o))
    rows[k] = acc.astype(BF16)

    def spread(source, c, piece=slice(None)):
        for o in plane_order:
            ref = rows.at[source, :, piece]
            push(ref, ref, gather_send, plane_recv.at[c], at_plane(o))

    for d in range(3, nz):
        hear(d)

    def offer(i, c):
        ref = rows.at[k, :, gather_parts[i]]
        push(ref, ref, gather_send, zed_recv.at[i, z], (c * ny + y, t))

    for i in range(len(gather_parts)):
        for d in reversed(range(1, nz)):
            pl.when(z + d < nz)(functools.partial(offer, i, z + d))
            pl.when(z >= d)(functools.partial(offer, i, z - d))
    spread(k, z)
    for h in range(heads):
        turned = factors[1, h].T
        for r in range(own):
            memory[r, h] = factors[0, h, r : r + 1] * memory[r, h] + turned[:, r : r + 1] * factors[2, h, r : r + 1]

    def chunk(j):
        return j - 1 + (nz + j - 1 - z) // nz if j else z

    def forward(j):
        c = chunk(j)
        for i, piece in enumerate(gather_parts):
            drain(rows.at[c * ny + y, :, piece], zed_recv.at[i, c])
            spread(c * ny + y, c, piece)

    gates = {}
    arrived(first + 1)
    arrived(first + 2)
    arrived(first + 3)

    def stage_a(c):
        if ny > 1:
            drain(rows.at[pl.ds(0, ny - 1)], plane_recv.at[chunk(c)])
        xf = rows[pl.ds(chunk(c) * ny, ny)].reshape(ny * own, cols).astype(F32)
        square = jnp.sum(xf * xf, axis=-1, keepdims=True)
        h = (xf * gain_ref[...]).astype(BF16)
        gate = nt_dot(h, w_gate[...])
        up = nt_dot(h, w_up[...])
        high = square.astype(BF16).astype(F32)
        lane = lax.broadcasted_iota(jnp.int32, (ny * own, 128), 1)
        part[c, :, 0:ff] = gate.astype(BF16)
        part[c, :, pad : pad + ff] = up.astype(BF16)
        part[c, :, 2 * pad :] = jnp.where(lane < 64, high, square - high).astype(BF16)
        for o in range(1, nt):
            push(part.at[c], part_in.at[c, o - 1], part_send, part_recv.at[c], at_tp(o))
        gates[c] = (gate, up, square)

    def stage_b(c):
        gate, up, square = gates.pop(c)
        if nt > 1:
            drain(part_in.at[c], part_recv.at[c])
        for o in range(1, nt):
            gate = gate + part_in[c, o - 1, :, 0:ff].astype(F32)
            up = up + part_in[c, o - 1, :, pad : pad + ff].astype(F32)
            tail = part_in[c, o - 1, :, 2 * pad :].astype(F32)
            square = square + jnp.sum(tail, axis=-1, keepdims=True) * (1.0 / 64)
        scale = lax.rsqrt(square / width + 1e-06)
        g = scale * gate
        hidden = (g / (1.0 + jnp.exp(-g)) * (scale * up)).astype(BF16)
        out = jnp.dot(hidden, w_down[...], preferred_element_type=F32)
        down[c] = out.reshape(ny, own, cols).astype(BF16)
        for i, piece in enumerate(reduce_parts):
            for o in plane_order:
                src, dst = down.at[c, partner(y, o), :, piece], down_in.at[c, o - 1, :, piece]
                push(src, dst, reduce_send, down_recv.at[i, c], at_plane(o))

    def stage_c(c):
        for i, piece in enumerate(reduce_parts):
            acc = down[c, y, :, piece].astype(F32)
            if ny > 1:
                drain(rows.at[pl.ds(0, ny - 1), :, piece], down_recv.at[i, c])
            for o in range(1, ny):
                acc = acc + down_in[c, o - 1, :, piece].astype(F32)
            if c == 0:
                ours[:, piece] = acc
            else:
                total[c, :, piece] = acc.astype(BF16)
                src, dst = total.at[c, :, piece], total_in.at[z, :, piece]
                push(src, dst, reduce_send, total_recv, (chunk(c) * ny + y, t))

    if nz > 1:
        forward(1)
    stage_a(0)
    for j in range(2, nz):
        forward(j)
    stage_b(0)
    if nz > 1:
        stage_a(1)
        stage_b(1)
    for j in range(2, nz + 1):
        if j < nz:
            stage_a(j)
        if j > 2:
            stage_b(j - 1)
    for j in range(1, nz):
        stage_c(j)
    stage_c(0)
    acc = rows[k].astype(F32) + ours[...]
    if nz > 1:
        drain(rows.at[pl.ds(0, nz - 1)], total_recv)
    for c in range(nz):
        acc = acc + total_in[c].astype(F32)
    out_ref[...] = acc.astype(BF16)
    if n > 1:
        drain(rows.at[pl.ds(0, n - 1)], gather_send)
        drain(rows.at[pl.ds(0, n - 1)], reduce_send)
    if nt > 1:
        drain(tok, tok_sem.at[1])
        drain(mix, mix_sem.at[1])
        drain(part_in, part_send)


def store_kernel(result, memory, normalizer, new_max, result_hbm, memory_hbm, normalizer_hbm, new_max_hbm, sem):
    pairs = [(memory, memory_hbm), (normalizer, normalizer_hbm), (new_max, new_max_hbm), (result, result_hbm)]
    copies = [pltpu.make_async_copy(src, dst, sem.at[i]) for i, (src, dst) in enumerate(pairs)]
    for copy in copies:
        copy.start()
    for copy in copies:
        copy.wait()


def per_device(
    mesh, tokens, norm_gain, w_query, w_key, w_value, w_outgate, w_input_gate, w_forget_gate,
    memory, normalizer, memory_max, w_output, ffn_gain, w_gate, w_up, w_down,
):
    n, nt = mesh.shape["kv"], mesh.shape["tp"]
    nz, ny = split_groups(n)
    own, cols = tokens.shape
    heads, dim = memory.shape[1], memory.shape[2]
    inner = heads * dim
    ff = w_down.shape[0]
    pad = -(-ff // 128) * 128
    dma = pltpu.SemaphoreType.DMA
    peers = max(nt - 1, 1)
    w_gate, w_up = w_gate.T, w_up.T
    vm = lambda like: pltpu.VMEM(like.shape, like.dtype)
    kept = 4 * (memory.size + 2 * normalizer.size) + 2 * tokens.size
    result, new_memory, new_normalizer, new_max = pl.pallas_call(
        functools.partial(step_kernel, nz, ny, nt, cols * nt),
        out_shape=(
            pltpu.VMEM((own, cols), BF16),
            pltpu.VMEM(memory.shape, F32),
            pltpu.VMEM(normalizer.shape, F32),
            pltpu.VMEM((heads, own), F32),
        ),
        in_specs=[HBM] * 16,
        out_specs=(VMEM,) * 4,
        scratch_shapes=[
            vm(tokens), pltpu.VMEM((1, cols * nt), F32), pltpu.VMEM(w_input_gate.shape[::-1], BF16),
            pltpu.VMEM(w_forget_gate.shape[::-1], BF16), vm(normalizer), pltpu.VMEM((heads, own), F32),
            pltpu.VMEM((1, cols), F32),
            vm(w_key), vm(w_value), vm(w_query), vm(w_outgate),
            vm(w_output), vm(w_gate), vm(w_up), vm(w_down),
            pltpu.VMEM((peers, own, cols), BF16),
            pltpu.VMEM((own, cols * nt), BF16),
            pltpu.VMEM((heads, own, dim), F32),
            pltpu.VMEM((3, heads, own, dim), F32),
            pltpu.VMEM((own, inner), BF16),
            pltpu.VMEM((peers, own, inner), BF16),
            pltpu.VMEM((n, own, cols), BF16),
            pltpu.VMEM((nz, ny * own, 2 * pad + 128), BF16),
            pltpu.VMEM((nz, peers, ny * own, 2 * pad + 128), BF16),
            pltpu.VMEM((nz, ny, own, cols), BF16),
            pltpu.VMEM((nz, max(ny - 1, 1), own, cols), BF16),
            pltpu.VMEM((nz, own, cols), BF16),
            pltpu.VMEM((nz, own, cols), BF16),
            pltpu.VMEM((own, cols), F32),
            dma((7,)),
            dma((DEPTH,)),
            dma((2,)),
            dma((2,)),
            dma((2, nz)),
            dma((nz,)),
            dma,
            dma((nz,)),
            dma,
            dma((2, nz)),
            dma,
            dma,
            pltpu.SemaphoreType.REGULAR((nz,)),
            pltpu.SemaphoreType.REGULAR((nz,)),
        ],
        compiler_params=pltpu.CompilerParams(collective_id=0, has_side_effects=True, vmem_limit_bytes=VMEM_BYTES - kept),
        name="decode_step",
    )(
        tokens, norm_gain.reshape(1, -1), w_input_gate.T, w_forget_gate.T, normalizer, memory_max.T,
        ffn_gain.reshape(1, cols), w_key, w_value, w_query, w_outgate, memory, w_output, w_gate, w_up, w_down,
    )
    result, new_memory, new_normalizer, new_max = pl.pallas_call(
        store_kernel,
        out_shape=(
            jax.ShapeDtypeStruct(tokens.shape, BF16),
            jax.ShapeDtypeStruct(memory.shape, F32),
            jax.ShapeDtypeStruct(normalizer.shape, F32),
            jax.ShapeDtypeStruct((heads, own), F32),
        ),
        in_specs=[VMEM] * 4,
        out_specs=(HBM,) * 4,
        scratch_shapes=[dma((4,))],
        compiler_params=pltpu.CompilerParams(vmem_limit_bytes=2**20),
        name="store",
    )(result, new_memory, new_normalizer, new_max)
    return (result, new_memory, new_normalizer, new_max.T)


def solution(mesh):
    placed = (
        P("kv", "tp"),
        P(),
        P(None, "tp"),
        P(None, "tp"),
        P(None, "tp"),
        P(None, "tp"),
        P(),
        P(),
        P("kv", "tp", None, None),
        P("kv", "tp", None),
        P("kv", "tp"),
        P(None, "tp"),
        P("tp"),
        P("tp", "kv"),
        P("tp", "kv"),
        P("kv", "tp"),
    )
    return jax.shard_map(
        functools.partial(per_device, mesh),
        mesh=mesh,
        in_specs=placed,
        out_specs=(P("kv", "tp"), P("kv", "tp", None, None), P("kv", "tp", None), P("kv", "tp")),
        check_vma=False,
    )
```

```python
import functools

import jax
import jax.numpy as jnp
from jax import lax
from jax.experimental import pallas as pl
from jax.experimental.pallas import tpu as pltpu
from jax.sharding import PartitionSpec as P

F32, BF16 = jnp.float32, jnp.bfloat16
MESH = pl.DeviceIdType.MESH
ANY = pl.BlockSpec(memory_space=pl.ANY)
VMEM = pl.BlockSpec(memory_space=pltpu.VMEM)
HBM = pl.BlockSpec(memory_space=pltpu.HBM)
DEPTH = 8
VMEM_BYTES = 67043328


def partner(index, bits):
    out, bit = index, 1
    while bit <= bits:
        if bits & bit:
            out = out + bit - 2 * bit * ((index // bit) % 2)
        bit *= 2
    return out


def split_groups(count):
    slow = 1
    while slow * slow < count:
        slow *= 2
    assert count % slow == 0
    return slow, count // slow


def parts_of(width, count):
    count = max(1, min(count, width // 128))
    step = width // count
    return [slice(i * step, (i + 1) * step) for i in range(count)]


def nt_dot(a, b):
    return lax.dot_general(a, b, (((1,), (1,)), ((), ())), preferred_element_type=F32)


def step_kernel(
    nz, ny, nt, width,
    tokens_hbm, norm_gain_hbm, w_ig_hbm, w_fg_hbm, normalizer_hbm, memory_max_hbm, gain_hbm,
    w_key_hbm, w_value_hbm, w_query_hbm, w_outgate_hbm, memory_hbm, w_out_hbm, w_gate_hbm, w_up_hbm, w_down_hbm,
    out_ref, memory, new_norm, new_max_ref,
    tokens_ref, norm_gain_ref, w_ig_ref, w_fg_ref, normalizer_ref, memory_max_ref, gain_ref,
    w_key, w_value, w_query, w_outgate, w_out, w_gate, w_up, w_down,
    tok, normed, num, factors, mixed_ref, mix, rows, part, part_in, down, down_in, total, total_in, ours,
    small_sem, load_sem, tok_sem, mix_sem, zed_recv, plane_recv, gather_send,
    part_recv, part_send, down_recv, total_recv, reduce_send, ahead_sem, behind_sem,
):
    k, t = lax.axis_index("kv"), lax.axis_index("tp")
    z, y = k // ny, k % ny
    n, own, cols = rows.shape
    heads, dim = memory.shape[1], memory.shape[3]
    ff = w_down.shape[0]
    pad = (part.shape[2] - 128) // 2
    gather_parts, reduce_parts = parts_of(cols, 2), parts_of(cols, 2)
    plane_order = sorted(range(1, ny), key=lambda o: -bin(o).count("1"))

    def at_plane(off):
        return (z * ny + partner(y, off), t)

    def at_tp(off):
        return (k, partner(t, off))

    smalls = [
        (tokens_hbm, tokens_ref), (norm_gain_hbm, norm_gain_ref), (w_ig_hbm, w_ig_ref), (w_fg_hbm, w_fg_ref),
        (memory_max_hbm, memory_max_ref), (normalizer_hbm, normalizer_ref), (gain_hbm, gain_ref),
    ]
    smalls = [pltpu.make_async_copy(src, dst, small_sem.at[i]) for i, (src, dst) in enumerate(smalls)]
    smalls[0].start()
    smalls[1].start()
    peers = [at_tp(o) for o in range(1, nt)]
    peers += [at_plane(o) for o in range(1, ny)]
    barrier = pltpu.get_barrier_semaphore()

    def at_step(d):
        return ((z + d) * ny + y, t)

    def greet(sem, device):
        pl.semaphore_signal(sem, inc=1, device_id=device, device_id_type=MESH)

    for peer in peers:
        greet(barrier, peer)
    if nz > 1:
        pl.when(z + 1 < nz)(lambda: greet(barrier, at_step(1)))
        pl.when(z >= 1)(lambda: greet(barrier, at_step(-1)))

    def tell(d):
        pl.when((z >= 1) & (z + d < nz))(lambda: greet(ahead_sem.at[d + 1], at_step(-1)))
        pl.when((z + 1 < nz) & (z >= d))(lambda: greet(behind_sem.at[d + 1], at_step(1)))

    def hear(d):
        pl.when(z + d < nz)(lambda: pl.semaphore_wait(ahead_sem.at[d], 1))
        pl.when(z >= d)(lambda: pl.semaphore_wait(behind_sem.at[d], 1))
        if d + 1 < nz:
            tell(d)

    pairs = [(w_query_hbm, w_query)]
    pairs += [(memory_hbm.at[:, h], memory.at[:, h]) for h in range(heads)]
    pairs += [(w_key_hbm, w_key), (w_value_hbm, w_value), (w_outgate_hbm, w_outgate)]
    pairs += [(w_out_hbm, w_out), (w_gate_hbm, w_gate), (w_up_hbm, w_up), (w_down_hbm, w_down)]
    loads = [pltpu.make_async_copy(src, dst, load_sem.at[i % DEPTH]) for i, (src, dst) in enumerate(pairs)]
    for load in loads[:1] + smalls[2:] + loads[1:DEPTH]:
        load.start()

    def arrived(i):
        loads[i].wait()
        if i + DEPTH < len(loads):
            loads[i + DEPTH].start()

    def push(src, dst, send_sem, recv_sem, device):
        pltpu.make_async_remote_copy(
            src_ref=src, dst_ref=dst, send_sem=send_sem, recv_sem=recv_sem,
            device_id=device, device_id_type=MESH,
        ).start()

    def drain(ref, sem):
        pltpu.make_async_copy(ref, ref, sem).wait()

    smalls[0].wait()
    pl.semaphore_wait(barrier, len(peers) + (2 * nz - 2 - z) // nz + (z + nz - 1) // nz)
    for o in range(1, nt):
        push(tokens_ref, tok.at[o - 1], tok_sem.at[1], tok_sem.at[0], at_tp(o))
    if nz > 2:
        tell(1)
    total_in[z] = jnp.zeros((own, cols), BF16)
    smalls[1].wait()
    if nt > 1:
        drain(tok, tok_sem.at[0])
    blocks = [(t, tokens_ref[...].astype(F32))]
    blocks += [(partner(t, o), tok[o - 1].astype(F32)) for o in range(1, nt)]
    square = jnp.sum(blocks[0][1] * blocks[0][1], axis=-1, keepdims=True)
    for _, block in blocks[1:]:
        square = square + jnp.sum(block * block, axis=-1, keepdims=True)
    row_scale = lax.rsqrt(square / width + 1e-06)
    for owner, block in blocks:
        at = pl.ds(pl.multiple_of(owner * cols, cols), cols)
        normed[:, at] = (block * row_scale * norm_gain_ref[:, at]).astype(BF16)
    x = normed[...]
    cut = [slice(h * dim, (h + 1) * dim) for h in range(heads)]

    def projected(i, weight):
        arrived(i)
        return jnp.dot(x, weight[...], preferred_element_type=F32)

    def recall(some):
        for h in some:
            turned = queries[:, cut[h]].T
            for r in range(own):
                num[h, r : r + 1, :] = jnp.sum(memory[r, h] * turned[:, r : r + 1], axis=0, keepdims=True)

    queries = projected(0, w_query) * dim ** (-0.5)
    for h in range(heads):
        arrived(1 + h)
    first = 1 + heads
    third = -(-heads // 3)
    keys = projected(first, w_key)
    recall(range(heads)[:third])
    values = projected(first + 1, w_value)
    recall(range(heads)[third : heads - heads // 3])
    if nz > 2:
        hear(2)
    for load in smalls[2:]:
        load.wait()
    outgates = projected(first + 2, w_outgate)
    recall(range(heads)[heads - heads // 3 :])
    igates, fgates = nt_dot(w_ig_ref[...], x), nt_dot(w_fg_ref[...], x)
    diagonal = lax.broadcasted_iota(jnp.int32, (own, own), 0) == lax.broadcasted_iota(jnp.int32, (own, own), 1)

    def along(row):
        return jnp.sum(jnp.where(diagonal, row, 0.0), axis=-1, keepdims=True)

    def mine(gates):
        picked = gates[0:heads]
        for i in range(1, nt):
            picked = jnp.where(t == i, gates[i * heads : (i + 1) * heads], picked)
        return picked

    igate, forget = mine(igates), mine(fgates)
    carried = jnp.minimum(forget, 0.0) - jnp.log1p(jnp.exp(-jnp.abs(forget))) + memory_max_ref[...]
    new_max = jnp.maximum(carried, igate)
    new_max_ref[...] = new_max
    keep_row, admit_row, floor_row = jnp.exp(carried - new_max), jnp.exp(igate - new_max), jnp.exp(-new_max)
    for h in range(heads):
        keep = jnp.broadcast_to(along(keep_row[h : h + 1]), (own, dim))
        key, value, query = along(admit_row[h : h + 1]) * keys[:, cut[h]], values[:, cut[h]], queries[:, cut[h]]
        factors[0, h], factors[1, h], factors[2, h] = keep, key, value
        grown = keep * normalizer_ref[:, h, :] + key
        new_norm[:, h, :] = grown
        denominator = jnp.sum(query * grown, axis=-1, keepdims=True)
        match = jnp.sum(query * key, axis=-1, keepdims=True)
        numerator = keep * num[h] + match * value
        cell_out = numerator / jnp.maximum(jnp.abs(denominator), along(floor_row[h : h + 1]))
        centered = cell_out - jnp.mean(cell_out, axis=-1, keepdims=True)
        head_var = jnp.mean(centered * centered, axis=-1, keepdims=True)
        gate = 1.0 / (1.0 + jnp.exp(-outgates[:, cut[h]]))
        mixed_ref[:, cut[h]] = (gate * centered * lax.rsqrt(head_var + 1e-05)).astype(BF16)

    for o in range(1, nt):
        push(mixed_ref, mix.at[o - 1], mix_sem.at[1], mix_sem.at[0], at_tp(o))
    first += 3
    arrived(first)
    inner = mixed_ref.shape[1]

    def project(value, owner):
        return jnp.dot(value, w_out[pl.ds(pl.multiple_of(owner * inner, inner), inner), :], preferred_element_type=F32)

    acc = tokens_ref[...].astype(F32) + project(mixed_ref[...], t)
    if nt > 1:
        drain(mix, mix_sem.at[0])
    for o in range(1, nt):
        acc = acc + project(mix[o - 1], partner(t, o))
    rows[k] = acc.astype(BF16)

    def spread(source, c, piece=slice(None)):
        for o in plane_order:
            ref = rows.at[source, :, piece]
            push(ref, ref, gather_send, plane_recv.at[c], at_plane(o))

    for d in range(3, nz):
        hear(d)

    def offer(i, c):
        ref = rows.at[k, :, gather_parts[i]]
        push(ref, ref, gather_send, zed_recv.at[i, z], (c * ny + y, t))

    for i in range(len(gather_parts)):
        for d in reversed(range(1, nz)):
            pl.when(z + d < nz)(functools.partial(offer, i, z + d))
            pl.when(z >= d)(functools.partial(offer, i, z - d))
    spread(k, z)
    for h in range(heads):
        turned = factors[1, h].T
        for r in range(own):
            memory[r, h] = factors[0, h, r : r + 1] * memory[r, h] + turned[:, r : r + 1] * factors[2, h, r : r + 1]

    def chunk(j):
        return j - 1 + (nz + j - 1 - z) // nz if j else z

    def forward(j):
        c = chunk(j)
        for i, piece in enumerate(gather_parts):
            drain(rows.at[c * ny + y, :, piece], zed_recv.at[i, c])
            spread(c * ny + y, c, piece)

    gates = {}
    arrived(first + 1)
    arrived(first + 2)
    arrived(first + 3)

    def share(c, span):
        for o in range(1, nt):
            push(part.at[c, :, span], part_in.at[c, o - 1, :, span], part_send, part_recv.at[c], at_tp(o))

    def stage_a(c):
        if ny > 1:
            drain(rows.at[pl.ds(0, ny - 1)], plane_recv.at[chunk(c)])
        xf = rows[pl.ds(chunk(c) * ny, ny)].reshape(ny * own, cols).astype(F32)
        square = jnp.sum(xf * xf, axis=-1, keepdims=True)
        h = (xf * gain_ref[...]).astype(BF16)
        gate = nt_dot(h, w_gate[...])
        part[c, :, 0:ff] = gate.astype(BF16)
        share(c, slice(0, pad))
        up = nt_dot(h, w_up[...])
        high = square.astype(BF16).astype(F32)
        lane = lax.broadcasted_iota(jnp.int32, (ny * own, 128), 1)
        part[c, :, pad : pad + ff] = up.astype(BF16)
        part[c, :, 2 * pad :] = jnp.where(lane < 64, high, square - high).astype(BF16)
        share(c, slice(pad, 2 * pad + 128))
        gates[c] = (gate, up, square)

    def stage_b(c):
        gate, up, square = gates.pop(c)
        if nt > 1:
            drain(part_in.at[c], part_recv.at[c])
        for o in range(1, nt):
            gate = gate + part_in[c, o - 1, :, 0:ff].astype(F32)
            up = up + part_in[c, o - 1, :, pad : pad + ff].astype(F32)
            tail = part_in[c, o - 1, :, 2 * pad :].astype(F32)
            square = square + jnp.sum(tail, axis=-1, keepdims=True) * (1.0 / 64)
        scale = lax.rsqrt(square / width + 1e-06)
        g = scale * gate
        hidden = (g / (1.0 + jnp.exp(-g)) * (scale * up)).astype(BF16)
        out = jnp.dot(hidden, w_down[...], preferred_element_type=F32)
        down[c] = out.reshape(ny, own, cols).astype(BF16)
        for i, piece in enumerate(reduce_parts):
            for o in plane_order:
                src, dst = down.at[c, partner(y, o), :, piece], down_in.at[c, o - 1, :, piece]
                push(src, dst, reduce_send, down_recv.at[i, c], at_plane(o))

    def stage_c(c):
        for i, piece in enumerate(reduce_parts):
            acc = down[c, y, :, piece].astype(F32)
            if ny > 1:
                drain(rows.at[pl.ds(0, ny - 1), :, piece], down_recv.at[i, c])
            for o in range(1, ny):
                acc = acc + down_in[c, o - 1, :, piece].astype(F32)
            if c == 0:
                ours[:, piece] = acc
            else:
                total[c, :, piece] = acc.astype(BF16)
                src, dst = total.at[c, :, piece], total_in.at[z, :, piece]
                push(src, dst, reduce_send, total_recv, (chunk(c) * ny + y, t))

    if nz > 1:
        forward(1)
    stage_a(0)
    for j in range(2, nz):
        forward(j)
    stage_b(0)
    if nz > 1:
        stage_a(1)
        stage_b(1)
    for j in range(2, nz + 1):
        if j < nz:
            stage_a(j)
        if j > 2:
            stage_b(j - 1)
    for j in range(1, nz):
        stage_c(j)
    stage_c(0)
    acc = rows[k].astype(F32) + ours[...]
    if nz > 1:
        drain(rows.at[pl.ds(0, nz - 1)], total_recv)
    for c in range(nz):
        acc = acc + total_in[c].astype(F32)
    out_ref[...] = acc.astype(BF16)
    if n > 1:
        drain(rows.at[pl.ds(0, n - 1)], gather_send)
        drain(rows.at[pl.ds(0, n - 1)], reduce_send)
    if nt > 1:
        drain(tok, tok_sem.at[1])
        drain(mix, mix_sem.at[1])
        drain(part_in, part_send)


def store_kernel(result, memory, normalizer, new_max, result_hbm, memory_hbm, normalizer_hbm, new_max_hbm, sem):
    pairs = [(memory, memory_hbm), (normalizer, normalizer_hbm), (new_max, new_max_hbm), (result, result_hbm)]
    copies = [pltpu.make_async_copy(src, dst, sem.at[i]) for i, (src, dst) in enumerate(pairs)]
    for copy in copies:
        copy.start()
    for copy in copies:
        copy.wait()


def per_device(
    mesh, tokens, norm_gain, w_query, w_key, w_value, w_outgate, w_input_gate, w_forget_gate,
    memory, normalizer, memory_max, w_output, ffn_gain, w_gate, w_up, w_down,
):
    n, nt = mesh.shape["kv"], mesh.shape["tp"]
    nz, ny = split_groups(n)
    own, cols = tokens.shape
    heads, dim = memory.shape[1], memory.shape[2]
    inner = heads * dim
    ff = w_down.shape[0]
    pad = -(-ff // 128) * 128
    dma = pltpu.SemaphoreType.DMA
    peers = max(nt - 1, 1)
    w_gate, w_up = w_gate.T, w_up.T
    vm = lambda like: pltpu.VMEM(like.shape, like.dtype)
    kept = 4 * (memory.size + 2 * normalizer.size) + 2 * tokens.size
    result, new_memory, new_normalizer, new_max = pl.pallas_call(
        functools.partial(step_kernel, nz, ny, nt, cols * nt),
        out_shape=(
            pltpu.VMEM((own, cols), BF16),
            pltpu.VMEM(memory.shape, F32),
            pltpu.VMEM(normalizer.shape, F32),
            pltpu.VMEM((heads, own), F32),
        ),
        in_specs=[HBM] * 16,
        out_specs=(VMEM,) * 4,
        scratch_shapes=[
            vm(tokens), pltpu.VMEM((1, cols * nt), F32), pltpu.VMEM(w_input_gate.shape[::-1], BF16),
            pltpu.VMEM(w_forget_gate.shape[::-1], BF16), vm(normalizer), pltpu.VMEM((heads, own), F32),
            pltpu.VMEM((1, cols), F32),
            vm(w_key), vm(w_value), vm(w_query), vm(w_outgate),
            vm(w_output), vm(w_gate), vm(w_up), vm(w_down),
            pltpu.VMEM((peers, own, cols), BF16),
            pltpu.VMEM((own, cols * nt), BF16),
            pltpu.VMEM((heads, own, dim), F32),
            pltpu.VMEM((3, heads, own, dim), F32),
            pltpu.VMEM((own, inner), BF16),
            pltpu.VMEM((peers, own, inner), BF16),
            pltpu.VMEM((n, own, cols), BF16),
            pltpu.VMEM((nz, ny * own, 2 * pad + 128), BF16),
            pltpu.VMEM((nz, peers, ny * own, 2 * pad + 128), BF16),
            pltpu.VMEM((nz, ny, own, cols), BF16),
            pltpu.VMEM((nz, max(ny - 1, 1), own, cols), BF16),
            pltpu.VMEM((nz, own, cols), BF16),
            pltpu.VMEM((nz, own, cols), BF16),
            pltpu.VMEM((own, cols), F32),
            dma((7,)),
            dma((DEPTH,)),
            dma((2,)),
            dma((2,)),
            dma((2, nz)),
            dma((nz,)),
            dma,
            dma((nz,)),
            dma,
            dma((2, nz)),
            dma,
            dma,
            pltpu.SemaphoreType.REGULAR((nz,)),
            pltpu.SemaphoreType.REGULAR((nz,)),
        ],
        compiler_params=pltpu.CompilerParams(collective_id=0, has_side_effects=True, vmem_limit_bytes=VMEM_BYTES - kept),
        name="decode_step",
    )(
        tokens, norm_gain.reshape(1, -1), w_input_gate.T, w_forget_gate.T, normalizer, memory_max.T,
        ffn_gain.reshape(1, cols), w_key, w_value, w_query, w_outgate, memory, w_output, w_gate, w_up, w_down,
    )
    result, new_memory, new_normalizer, new_max = pl.pallas_call(
        store_kernel,
        out_shape=(
            jax.ShapeDtypeStruct(tokens.shape, BF16),
            jax.ShapeDtypeStruct(memory.shape, F32),
            jax.ShapeDtypeStruct(normalizer.shape, F32),
            jax.ShapeDtypeStruct((heads, own), F32),
        ),
        in_specs=[VMEM] * 4,
        out_specs=(HBM,) * 4,
        scratch_shapes=[dma((4,))],
        compiler_params=pltpu.CompilerParams(vmem_limit_bytes=2**20),
        name="store",
    )(result, new_memory, new_normalizer, new_max)
    return (result, new_memory, new_normalizer, new_max.T)


def solution(mesh):
    placed = (
        P("kv", "tp"),
        P(),
        P(None, "tp"),
        P(None, "tp"),
        P(None, "tp"),
        P(None, "tp"),
        P(),
        P(),
        P("kv", "tp", None, None),
        P("kv", "tp", None),
        P("kv", "tp"),
        P(None, "tp"),
        P("tp"),
        P("tp", "kv"),
        P("tp", "kv"),
        P("kv", "tp"),
    )
    return jax.shard_map(
        functools.partial(per_device, mesh),
        mesh=mesh,
        in_specs=placed,
        out_specs=(P("kv", "tp"), P("kv", "tp", None, None), P("kv", "tp", None), P("kv", "tp")),
        check_vma=False,
    )
```
